32 devices in a mesh: sp: 4 (over y, x), dp: 8 (over z, core).
Axes of the slice: x: 2, y: 2, z: 4, core: 2. Of those that a mesh axis runs over, the one named last changes fastest.
Arguments:
- tokens: bfloat16 [8, 1536, 2048], P('dp', 'sp'), may hold values from -6 to 6
- value_act: bfloat16 [8, 1536, 1024], P('dp', 'sp'), may hold values from -6 to 6
- gate_act: bfloat16 [8, 1536, 1024], P('dp', 'sp'), may hold values from -6 to 6
- cotangent: bfloat16 [8, 1536, 1024], P('dp', 'sp'), may hold values from -6 to 6
- value_weight: bfloat16 [2048, 1024], P('dp'), may hold values from -0.1875 to 0.1875
- gate_weight: bfloat16 [2048, 1024], P('dp'), may hold values from -0.1875 to 0.1875
- norm_gain: float32 [1024], replicated, may hold values from 0.1 to 1.9
- norm_bias: float32 [1024], replicated, may hold values from -3 to 3
- mix_weight: bfloat16 [16, 128, 128], replicated, may hold values from -0.5 to 0.5
- mix_bias: float32 [16, 128], replicated, may hold values from 0.1 to 1.9
Outputs:
- tokens_grad: bfloat16 [8, 1536, 2048], P('dp', 'sp')
- value_weight_grad: float32 [2048, 1024], P('dp')
- gate_weight_grad: float32 [2048, 1024], P('dp')
- mix_weight_grad: float32 [16, 128, 128], replicated
- mix_bias_grad: float32 [16, 128], replicated
- norm_gain_grad: float32 [1024], replicated
- norm_bias_grad: float32 [1024], replicated
The draws below stay inside these ranges and needn't reach their ends.
All inputs are finite; a program needn't handle non-finite values.
Results may differ from the reference program's by a relative error of at most 0.0054.
Values may be sent and summed in bfloat16 or wider, within the bound.
A program may use at most 128 MiB of HBM per device.

```python
import jax
import jax.numpy as jnp
from jax import lax

D = 2048
GROUPS = 16
DG = 1024
BLOCK = 128
SEQ = 1536
SEQS = 8


def strengthened(array, stream_key, source, target, parts, factor):
    owner, partner = [(jnp.arange(array.shape[dim]) // (array.shape[dim] // parts)).reshape([-1 if axis == dim else 1 for axis in range(array.ndim)]) for dim in (source, target)]
    chosen = jax.random.permutation(stream_key, parts)[partner]
    strong = (owner == chosen) | (owner == (partner + parts // 2) % parts)
    return jnp.where(strong, factor * array, array)


def block_scale(rng, shape, split, least, high):
    level, own = 1.0, jax.random.fold_in(rng, 6)
    for axis_at, parts in split:
        steps = jnp.exp(jax.random.uniform(jax.random.fold_in(own, axis_at), (parts,), jnp.float32, least / len(split), high / len(split)))
        level = level * jnp.repeat(steps, shape[axis_at] // parts).reshape([-1 if axis == axis_at else 1 for axis in range(len(shape))])
    return level


def scatter_about(stream_key, dims, scale, bound, split=(), kind=jnp.bfloat16):
    loudness = block_scale(stream_key, dims, split, -0.22, 0.18) if split else 1.0
    values = jax.random.normal(stream_key, dims, jnp.float32) * scale * loudness
    return jnp.minimum(jnp.maximum(values, -bound), bound).astype(kind)


def noise_with(stream_key, dims, spread, most, shards, heavy, kind=jnp.bfloat16):
    array = spread * jax.random.normal(stream_key, dims, jnp.float32)
    if shards:
        array = array * block_scale(stream_key, dims, shards, -0.22, 0.18)
    return jnp.clip(strengthened(array, jax.random.fold_in(stream_key, 3), *heavy), -most, most).astype(kind)


def setup_inputs(seed: int = 0) -> dict:
    key_of = jax.random.split(jax.random.key(seed), 11)
    tokens = noise_with(key_of[0], (SEQS, SEQ, D), 1.0, 6.0, ((0, 8), (1, 4)), (1, 2, 4, 2.0))
    value_act = scatter_about(key_of[1], (SEQS, SEQ, DG), 1.0, 6.0, ((0, 8), (1, 4)))
    gate_act = scatter_about(key_of[2], (SEQS, SEQ, DG), 1.0, 6.0, ((0, 8), (1, 4)))
    cotangent = scatter_about(key_of[3], (SEQS, SEQ, DG), 1.0, 6.0, ((0, 8), (1, 4)))
    value_weight = scatter_about(key_of[4], (D, DG), DG ** -0.5, 0.1875, ((0, 8),))
    gate_weight = scatter_about(key_of[5], (D, DG), DG ** -0.5, 0.1875, ((0, 8),))
    norm_gain = jnp.clip(1.0 + 0.18 * jax.random.normal(key_of[6], (DG,), jnp.float32), 0.1, 1.9)
    norm_bias = scatter_about(key_of[7], (DG,), 0.5, 3.0, (), jnp.float32)
    mix_weight = scatter_about(key_of[8], (GROUPS, BLOCK, BLOCK), BLOCK ** -0.5, 0.5)
    mix_bias = jnp.clip(1.0 + 0.18 * jax.random.normal(key_of[9], (GROUPS, BLOCK), jnp.float32), 0.1, 1.9)
    return {"tokens": tokens, "value_act": value_act, "gate_act": gate_act, "cotangent": cotangent, "value_weight": value_weight, "gate_weight": gate_weight, "norm_gain": norm_gain, "norm_bias": norm_bias, "mix_weight": mix_weight, "mix_bias": mix_bias}


EPSILON = 1e-06

def gelu_slope(values):
    cdf_part = 0.5 * (1.0 + lax.erf(values * 0.7071067811865476))
    pdf_part = jnp.exp(-0.5 * values * values) * 0.3989422804014327
    return cdf_part + values * pdf_part

def mixer_backward(value_act, gate_act, cotangent, norm_gain, norm_bias, mix_weight, mix_bias):
    seq_len, channels = value_act.shape
    groups, block_len = (mix_weight.shape[0], mix_weight.shape[1])
    group_dim = channels // groups
    blocks = seq_len // block_len
    value_float = value_act.astype(jnp.float32)
    gate_float = gate_act.astype(jnp.float32)
    activated = jax.nn.gelu(value_float, approximate=False)
    gate_gelu = jax.nn.gelu(gate_float, approximate=False)
    centred = gate_gelu - lax.optimization_barrier(jnp.mean(gate_gelu, axis=-1, keepdims=True))
    inv_std = lax.rsqrt(lax.optimization_barrier(jnp.mean(centred * centred, axis=-1, keepdims=True)) + EPSILON)
    normed = centred * inv_std
    spread_in = (normed * norm_gain + norm_bias).astype(jnp.bfloat16)
    spread_in = spread_in.reshape(blocks, block_len, groups, group_dim)
    causal = jnp.tril(jnp.ones((block_len, block_len), dtype=bool))
    masked_weight = jnp.where(causal[None], mix_weight, jnp.zeros_like(mix_weight))
    spatial = jnp.einsum('gts,bsgd->btgd', masked_weight.astype(jnp.float32), spread_in.astype(jnp.float32))
    spatial = (spatial + mix_bias.T[None, :, :, None]).reshape(seq_len, channels)
    grad_out = cotangent.astype(jnp.float32)
    grad_act = grad_out * spatial
    grad_spatial = grad_out * activated
    grad_split = grad_spatial.reshape(blocks, block_len, groups, group_dim)
    bias_grad = lax.optimization_barrier(jnp.sum(grad_split, axis=(0, 3))).T
    spatial_low = grad_split.astype(jnp.bfloat16)
    weight_grad = jnp.einsum('btgd,bsgd->gts', spatial_low.astype(jnp.float32), spread_in.astype(jnp.float32))
    weight_grad = jnp.where(causal[None], weight_grad, jnp.zeros_like(weight_grad))
    grad_norm = jnp.einsum('gts,btgd->bsgd', masked_weight.astype(jnp.float32), spatial_low.astype(jnp.float32))
    grad_norm = grad_norm.reshape(seq_len, channels)
    gain_grad = lax.optimization_barrier(jnp.sum(grad_norm * normed, axis=0))
    shift_grad = lax.optimization_barrier(jnp.sum(grad_norm, axis=0))
    grad_hat = grad_norm * norm_gain
    grad_gate = inv_std * (grad_hat - lax.optimization_barrier(jnp.mean(grad_hat, axis=-1, keepdims=True)) - normed * lax.optimization_barrier(jnp.mean(grad_hat * normed, axis=-1, keepdims=True)))
    value_grad = (grad_act * gelu_slope(value_float)).astype(jnp.bfloat16)
    gate_grad = (grad_gate * gelu_slope(gate_float)).astype(jnp.bfloat16)
    return (value_grad, gate_grad, (weight_grad, bias_grad, gain_grad, shift_grad))

def reference(tokens, value_act, gate_act, cotangent, value_weight, gate_weight, norm_gain, norm_bias, mix_weight, mix_bias):
    both_weights = jnp.concatenate((value_weight, gate_weight), axis=1)

    def per_sequence(running, seq_items):
        inputs, value_seq, gate_seq, cot_seq = seq_items
        value_grad, gate_grad, stats = mixer_backward(value_seq, gate_seq, cot_seq, norm_gain, norm_bias, mix_weight, mix_bias)
        both_grads = jnp.concatenate((value_grad, gate_grad), axis=1)
        input_grad = jnp.dot(both_grads, both_weights.T, preferred_element_type=jnp.float32).astype(jnp.bfloat16)
        weight_sums = running[0] + jnp.dot(inputs.T, both_grads, preferred_element_type=jnp.float32)
        updated = (weight_sums,) + tuple((old + term for old, term in zip(running[1:], stats)))
        return (updated, input_grad)
    initial = (jnp.zeros((D, 2 * DG), jnp.float32), jnp.zeros((GROUPS, BLOCK, BLOCK), jnp.float32), jnp.zeros((GROUPS, BLOCK), jnp.float32), jnp.zeros((DG,), jnp.float32), jnp.zeros((DG,), jnp.float32))
    running, input_grads = lax.scan(per_sequence, initial, (tokens, value_act, gate_act, cotangent))
    return (input_grads, running[0][:, :DG], running[0][:, DG:], running[1], running[2], running[3], running[4])
```

```python
import functools

import jax
import jax.numpy as jnp
from jax import lax
from jax.experimental import pallas as pl
from jax.experimental.pallas import tpu as pltpu
from jax.sharding import PartitionSpec as P

EPSILON = 1e-06
CORES = 2
MESH = pl.DeviceIdType.MESH
F32 = jnp.float32
BF16 = jnp.bfloat16


def remote(src, dst, send, recv, device):
    return pltpu.make_async_remote_copy(
        src_ref=src, dst_ref=dst, send_sem=send, recv_sem=recv, device_id=device, device_id_type=MESH
    )


def position():
    s, d = lax.axis_index("sp"), lax.axis_index("dp")
    return s, d, d // CORES, d % CORES


def greet(ways, levels, s, d, z, c):
    barrier = pltpu.get_barrier_semaphore()
    for k in range(1, ways):
        pl.semaphore_signal(barrier, inc=1, device_id=((s + k) % ways, d), device_id_type=MESH)
    for k in range(1, levels):
        other = ((z + k) % levels) * CORES + c
        pl.semaphore_signal(barrier, inc=1, device_id=(s, other), device_id_type=MESH)
    pl.semaphore_signal(barrier, inc=1, device_id=(s, d + 1 - 2 * c), device_id_type=MESH)
    pl.semaphore_wait(barrier, ways - 1 + levels - 1 + 1)


def phi(values):
    cdf_part = 0.5 * (1.0 + lax.erf(values * 0.7071067811865476))
    pdf_part = jnp.exp(-0.5 * values * values) * 0.3989422804014327
    return cdf_part, cdf_part + values * pdf_part


def mix_kernel(
    ways, levels,
    tokens, weights, value_act, gate_act, cotangent, gain, shift, mix, mix_turned, bias,
    both, pair_tokens, pair_grads, gathered, weight_grad, spatial_sum, gain_grad, shift_grad,
    own_part, swap_part, spread, low, spatial, grad_norm,
    local_sem, core_sem, level_sem, plane_sem, relay_sem,
):
    s, d, z, c = position()
    partner = (s, d + 1 - 2 * c)
    seq_len, channels = value_act.shape
    pairs, double, block_len = mix.shape
    lanes = channels // pairs
    width = weights.shape[1]
    piece = width // ways

    def columns(index):
        return pl.ds(pl.multiple_of(index * piece, piece), piece)

    greet(ways, levels, s, d, z, c)
    level_copies = []
    for k in range(1, levels):
        level_copies.append(remote(
            weights.at[:, columns(s)], gathered.at[z, c, :, columns(s)],
            level_sem.at[0, k - 1], level_sem.at[1, k - 1],
            (s, ((z + k) % levels) * CORES + c),
        ))
    order = sorted(range(levels - 1), key=lambda k: min(k + 1, levels - 1 - k))
    for k in order:
        level_copies[k].start()
    token_swap = remote(tokens, pair_tokens.at[1], core_sem.at[0, 0], core_sem.at[1, 0], partner)
    token_swap.start()
    shard_swap = remote(weights, gathered.at[z, c], core_sem.at[0, 1], core_sem.at[1, 1], partner)
    shard_swap.start()
    token_copy = pltpu.make_async_copy(tokens, pair_tokens.at[0], local_sem.at[0])
    token_copy.start()
    shard_copy = pltpu.make_async_copy(weights, gathered.at[z, c], local_sem.at[1])
    shard_copy.start()

    plane_copies, relays = {}, {}

    def forward(k):
        level_copies[k].wait_recv()
        source = (z + levels - 1 - k) % levels
        block = gathered.at[source, c, :, columns(s)]
        for j in range(1, ways):
            copy = remote(
                block, block, plane_sem.at[0, k, j - 1], plane_sem.at[1, k, j - 1], ((s + j) % ways, d)
            )
            copy.start()
            plane_copies[k, j] = copy
        relay = remote(block, block, relay_sem.at[0, k, 0], relay_sem.at[1, k, 0], partner)
        relay.start()
        relays[k, 0] = relay

    def relay_plane(k, j):
        plane_copies[k, j].wait_recv()
        source = (z + levels - 1 - k) % levels
        block = gathered.at[source, c, :, columns((s + ways - j) % ways)]
        relay = remote(block, block, relay_sem.at[0, k, j], relay_sem.at[1, k, j], partner)
        relay.start()
        relays[k, j] = relay

    weight_grad[...] = jnp.zeros_like(weight_grad)
    spatial_sum[...] = jnp.zeros_like(spatial_sum)
    gain_grad[...] = jnp.zeros_like(gain_grad)
    shift_grad[...] = jnp.zeros_like(shift_grad)
    first_half = lax.broadcasted_iota(jnp.int32, (block_len, lanes), 1) < lanes // 2
    waiting = list(order)
    blocks = seq_len // block_len
    for b in range(blocks):
        rows = pl.ds(b * block_len, block_len)
        gate = gate_act[rows, :].astype(F32)
        gate_cdf, gate_slope = phi(gate)
        gelu = gate * gate_cdf
        centred = gelu - jnp.mean(gelu, axis=-1, keepdims=True)
        inv_std = lax.rsqrt(jnp.mean(centred * centred, axis=-1, keepdims=True) + EPSILON)
        normed = centred * inv_std
        spread[...] = (normed * gain[...] + shift[...]).astype(BF16)
        value = value_act[rows, :].astype(F32)
        value_cdf, value_slope = phi(value)
        grad_out = cotangent[rows, :].astype(F32)
        grad_spatial = grad_out * (value * value_cdf)
        spatial_sum[...] += grad_spatial
        low[...] = grad_spatial.astype(BF16)
        for p in range(pairs):
            cut = pl.ds(p * lanes, lanes)
            inner = spread[:, cut]
            mixed = jnp.dot(mix[p], inner, preferred_element_type=F32)
            spatial[:, cut] = jnp.where(first_half, mixed[:block_len], mixed[block_len:]) + bias[:, cut]
            piece_low = low[:, cut]
            zero = jnp.zeros_like(piece_low)
            apart = jnp.concatenate(
                (jnp.where(first_half, piece_low, zero), jnp.where(first_half, zero, piece_low)), axis=0
            )
            weight_grad[p] += lax.dot_general(
                apart, inner, (((1,), (1,)), ((), ())), preferred_element_type=F32
            )
            grad_norm[:, cut] = jnp.dot(mix_turned[p], apart, preferred_element_type=F32)
        back = grad_norm[...]
        gain_grad[...] += jnp.sum(back * normed, axis=0, keepdims=True)
        shift_grad[...] += jnp.sum(back, axis=0, keepdims=True)
        hat = back * gain[...]
        grad_gate = inv_std * (
            hat
            - jnp.mean(hat, axis=-1, keepdims=True)
            - normed * jnp.mean(hat * normed, axis=-1, keepdims=True)
        )
        value_grad = (grad_out * spatial[...] * value_slope).astype(BF16)
        gate_grad = (grad_gate * gate_slope).astype(BF16)
        both[rows, :channels] = value_grad
        both[rows, channels:] = gate_grad
        chosen = jnp.full(value_grad.shape, c, jnp.int32) == 0
        own_part[rows, :] = jnp.where(chosen, value_grad.astype(F32), gate_grad.astype(F32)).astype(BF16)
        swap_part[rows, :] = jnp.where(chosen, gate_grad.astype(F32), value_grad.astype(F32)).astype(BF16)
        if waiting and b < blocks - 1:
            forward(waiting.pop(0))
    grad_copy = pltpu.make_async_copy(own_part, pair_grads.at[0], local_sem.at[2])
    grad_copy.start()
    grad_swap = remote(swap_part, pair_grads.at[1], core_sem.at[0, 2], core_sem.at[1, 2], partner)
    grad_swap.start()
    while waiting:
        forward(waiting.pop(0))
    for k in order:
        for j in range(1, ways):
            relay_plane(k, j)
    token_copy.wait()
    shard_copy.wait()
    grad_copy.wait()
    for copy in level_copies:
        copy.wait_send()
    for key in plane_copies:
        plane_copies[key].wait_send()
    for copy in (token_swap, shard_swap, grad_swap):
        copy.wait()
    for key in relays:
        relays[key].wait()


def sum_kernel(
    ways, levels,
    part, mix_part, small,
    summed, mix_out, small_out,
    plane_in, level_out, level_in, own_sum, final, final_in,
    mix_in, mix_low, mix_plane, mix_sum, mix_level_out, mix_level, small_in, small_plane, small_level,
    core_sem, plane_sem, level_sem, gather_sem, mix_sem, mix_level_sem, mix_up_sem, mix_out_sem,
    small_sem, small_level_sem,
):
    s, d, z, c = position()
    partner = (s, d + 1 - 2 * c)
    half = part.shape[-1]

    def in_plane(k):
        return ((s + k) % ways, d)

    def in_level(k):
        return (s, ((z + k) % levels) * CORES + c)

    greet(ways, levels, s, d, z, c)
    mix_swap = remote(mix_part.at[1 - c], mix_in, core_sem.at[0, 0], core_sem.at[1, 0], partner)
    mix_swap.start()
    small_swap = remote(small, small_in, core_sem.at[0, 1], core_sem.at[1, 1], partner)
    small_swap.start()
    copies = {}

    def send_chunk(i):
        target = (z + 1 + i) % levels
        for k in range(1, ways):
            copy = remote(
                part.at[target, :, (s + k) % ways], plane_in.at[i, k - 1],
                plane_sem.at[0, i, k - 1], plane_sem.at[1, i, k - 1], in_plane(k),
            )
            copy.start()
            copies[i, k] = copy

    pending = []

    send_chunk(0)
    mix_swap.wait()
    small_swap.wait()
    mix_low[...] = (mix_part[c] + mix_in[...]).astype(BF16)
    small_plane[s] = small[...] + small_in[...]
    mix_copies, small_copies = [], []
    for k in range(1, ways):
        mix_copies.append(remote(
            mix_low.at[(s + k) % ways], mix_plane.at[k - 1],
            mix_sem.at[0, k - 1], mix_sem.at[1, k - 1], in_plane(k),
        ))
        small_copies.append(remote(
            small_plane.at[s], small_plane.at[s],
            small_sem.at[0, k - 1], small_sem.at[1, k - 1], in_plane(k),
        ))
    for copy in mix_copies + small_copies:
        copy.start()
    for i in range(1, levels):
        send_chunk(i)

    mix_level_copies, small_level_copies, mix_up, mix_gather = [], [], [], []

    def mix_stage(stage):
        if stage == 0:
            for copy in mix_copies + small_copies:
                copy.wait()
            total = mix_low[s].astype(F32)
            for k in range(1, ways):
                total = total + mix_plane[k - 1].astype(F32)
            mix_sum[...] = total
            mix_level_out[...] = total.astype(BF16)
            gathered = small_plane[0]
            for k in range(1, ways):
                gathered = gathered + small_plane[k]
            small_level[z] = gathered
            for k in range(1, levels):
                mix_level_copies.append(remote(
                    mix_level_out.at[(z + k) % levels], mix_level.at[k - 1],
                    mix_level_sem.at[0, k - 1], mix_level_sem.at[1, k - 1], in_level(k),
                ))
                small_level_copies.append(remote(
                    small_level.at[z], small_level.at[z],
                    small_level_sem.at[0, k - 1], small_level_sem.at[1, k - 1], in_level(k),
                ))
            for copy in mix_level_copies + small_level_copies:
                copy.start()
        elif stage == 1:
            for copy in mix_level_copies + small_level_copies:
                copy.wait()
            total = mix_sum[z]
            for k in range(1, levels):
                total = total + mix_level[k - 1].astype(F32)
            mix_out[c, s, z] = total.astype(BF16)
            gathered = small_level[0]
            for k in range(1, levels):
                gathered = gathered + small_level[k]
            small_out[...] = gathered
            for k in range(1, levels):
                block = mix_out.at[c, s, z]
                mix_up.append(remote(
                    block, block, mix_up_sem.at[0, k - 1], mix_up_sem.at[1, k - 1], in_level(k)
                ))
                mix_up[-1].start()
        else:
            for copy in mix_up:
                copy.wait()
            for k in range(1, ways):
                block = mix_out.at[c, s]
                mix_gather.append(remote(
                    block, block, mix_out_sem.at[0, k - 1], mix_out_sem.at[1, k - 1], in_plane(k)
                ))
                mix_gather[-1].start()

    stages = [0, 1, 2]
    level_copies = []
    for i in range(levels):
        target = (z + 1 + i) % levels
        total = part[target, :, s].astype(F32)
        for k in range(1, ways):
            copies[i, k].wait_recv()
            total = total + plane_in[i, k - 1].astype(F32)
        if i < levels - 1:
            level_out[i] = total.astype(BF16)
            copy = remote(
                level_out.at[i], level_in.at[i], level_sem.at[0, i], level_sem.at[1, i], in_level(i + 1)
            )
            copy.start()
            level_copies.append(copy)
            if stages:
                mix_stage(stages.pop(0))
        else:
            own_sum[...] = total
    total = own_sum[...]
    for i in range(levels - 1):
        level_copies[i].wait_recv()
        total = total + level_in[i].astype(F32)
    final[...] = total
    final_swap = remote(final.at[1 - c], final_in, core_sem.at[0, 2], core_sem.at[1, 2], partner)
    final_swap.start()
    while stages:
        mix_stage(stages.pop(0))
    final_swap.wait()
    mine, theirs = final[c], final_in[...]
    lower = jnp.full(mine.shape, c, jnp.int32) == 0
    summed[s, :, :half] = jnp.where(lower, mine, theirs).astype(BF16)
    summed[s, :, half:] = jnp.where(lower, theirs, mine).astype(BF16)
    gather = []
    for k in range(1, ways):
        copy = remote(
            summed.at[s], summed.at[s], gather_sem.at[0, k - 1], gather_sem.at[1, k - 1], in_plane(k)
        )
        copy.start()
        gather.append(copy)
    for copy in mix_gather:
        copy.wait()
    mix_back = remote(mix_out.at[c], mix_out.at[c], core_sem.at[0, 3], core_sem.at[1, 3], partner)
    mix_back.start()
    mix_back.wait()
    for copy in gather:
        copy.wait()
    for copy in level_copies:
        copy.wait_send()
    for key in copies:
        copies[key].wait_send()


def shards(
    tokens,
    value_act,
    gate_act,
    cotangent,
    value_weight,
    gate_weight,
    norm_gain,
    norm_bias,
    mix_weight,
    mix_bias,
):
    ways = lax.axis_size("sp")
    levels = lax.axis_size("dp") // CORES
    inputs = tokens[0]
    seq_len, width = inputs.shape
    channels = value_act.shape[2]
    groups, block_len = mix_weight.shape[0], mix_weight.shape[1]
    group_dim = channels // groups
    pairs = groups // 2
    rows = value_weight.shape[0]
    vmem = pl.BlockSpec(memory_space=pltpu.VMEM)
    hbm = pl.BlockSpec(memory_space=pl.ANY)
    sems = pltpu.SemaphoreType.DMA
    weights = jnp.concatenate((value_weight, gate_weight), axis=1)
    causal = jnp.tril(jnp.ones((block_len, block_len), dtype=bool))
    masked = jnp.where(causal[None], mix_weight, jnp.zeros_like(mix_weight))
    mix = masked.reshape(pairs, 2 * block_len, block_len)
    bias = jnp.repeat(mix_bias.T, group_dim, axis=1)
    shape = jax.ShapeDtypeStruct
    both, pair_tokens, pair_grads, gathered, weight_grad, spatial_sum, gain_grad, shift_grad = pl.pallas_call(
        functools.partial(mix_kernel, ways, levels),
        out_shape=(
            shape((seq_len, 2 * channels), BF16),
            shape((CORES, seq_len, width), BF16),
            shape((CORES, seq_len, channels), BF16),
            shape((levels, CORES, rows, 2 * channels), BF16),
            shape((pairs, 2 * block_len, block_len), F32),
            shape((block_len, channels), F32),
            shape((1, channels), F32),
            shape((1, channels), F32),
        ),
        in_specs=[vmem] * 10,
        out_specs=(vmem, hbm, hbm, hbm, vmem, vmem, vmem, vmem),
        scratch_shapes=[
            pltpu.VMEM((seq_len, channels), BF16),
            pltpu.VMEM((seq_len, channels), BF16),
            pltpu.VMEM((block_len, channels), BF16),
            pltpu.VMEM((block_len, channels), BF16),
            pltpu.VMEM((block_len, channels), F32),
            pltpu.VMEM((block_len, channels), F32),
            sems((3,)),
            sems((2, 3)),
            sems((2, levels - 1)),
            sems((2, levels - 1, ways - 1)),
            sems((2, levels - 1, ways)),
        ],
        compiler_params=pltpu.CompilerParams(
            collective_id=0, has_side_effects=True, vmem_limit_bytes=40 * 1024 * 1024
        ),
        name="mix",
    )(
        inputs, weights, value_act[0], gate_act[0], cotangent[0],
        norm_gain[None], norm_bias[None], mix, mix.transpose(0, 2, 1), bias,
    )
    part = lax.dot_general(
        pair_tokens.reshape(CORES * seq_len, width),
        pair_grads.reshape(CORES * seq_len, channels),
        (((0,), (0,)), ((), ())),
        preferred_element_type=F32,
    ).astype(BF16)
    share = rows // ways
    part = part.reshape(levels, CORES, ways, share, channels)
    low_rows = groups * block_len // (CORES * ways * levels)
    mix_part = weight_grad.reshape(CORES, ways, levels, low_rows, block_len)
    bias_grad = jnp.sum(spatial_sum.reshape(block_len, groups, group_dim), axis=-1).T
    lanes = 128
    small = jnp.concatenate((bias_grad.reshape(-1), gain_grad[0], shift_grad[0])).reshape(-1, lanes)
    input_grad = lax.dot_general(
        both, gathered.reshape(width, 2 * channels), (((1,), (1,)), ((), ())), preferred_element_type=F32
    ).astype(BF16)
    summed, mix_out, small_out = pl.pallas_call(
        functools.partial(sum_kernel, ways, levels),
        out_shape=(
            shape((ways, share, 2 * channels), BF16),
            shape(mix_part.shape, BF16),
            shape(small.shape, F32),
        ),
        in_specs=[vmem] * 3,
        out_specs=(vmem,) * 3,
        scratch_shapes=[
            pltpu.VMEM((levels, ways - 1, CORES, share, channels), BF16),
            pltpu.VMEM((levels - 1, CORES, share, channels), BF16),
            pltpu.VMEM((levels - 1, CORES, share, channels), BF16),
            pltpu.VMEM((CORES, share, channels), F32),
            pltpu.VMEM((CORES, share, channels), F32),
            pltpu.VMEM((share, channels), F32),
            pltpu.VMEM(mix_part.shape[1:], F32),
            pltpu.VMEM(mix_part.shape[1:], BF16),
            pltpu.VMEM((ways - 1,) + mix_part.shape[2:], BF16),
            pltpu.VMEM(mix_part.shape[2:], F32),
            pltpu.VMEM(mix_part.shape[2:], BF16),
            pltpu.VMEM((levels - 1,) + mix_part.shape[3:], BF16),
            pltpu.VMEM(small.shape, F32),
            pltpu.VMEM((ways,) + small.shape, F32),
            pltpu.VMEM((levels,) + small.shape, F32),
            sems((2, 4)),
            sems((2, levels, ways - 1)),
            sems((2, levels - 1)),
            sems((2, ways - 1)),
            sems((2, ways - 1)),
            sems((2, levels - 1)),
            sems((2, levels - 1)),
            sems((2, ways - 1)),
            sems((2, ways - 1)),
            sems((2, levels - 1)),
        ],
        compiler_params=pltpu.CompilerParams(
            collective_id=1, has_side_effects=True, vmem_limit_bytes=48 * 1024 * 1024
        ),
        name="sum",
    )(part, mix_part, small)
    weight_sums = summed.reshape(rows, 2 * channels).astype(F32)
    mix_grad = jnp.where(causal[None], mix_out.reshape(groups, block_len, block_len).astype(F32), 0.0)
    small_out = small_out.reshape(-1)
    biases = groups * block_len
    return (
        input_grad[None],
        weight_sums[:, :channels],
        weight_sums[:, channels:],
        mix_grad,
        small_out[:biases].reshape(groups, block_len),
        small_out[biases:biases + channels],
        small_out[biases + channels:],
    )


def solution(mesh):
    placed = (
        P("dp", "sp", None),
        P("dp", "sp", None),
        P("dp", "sp", None),
        P("dp", "sp", None),
        P("dp", None),
        P("dp", None),
        P(),
        P(),
        P(),
        P(),
    )
    return jax.shard_map(
        shards,
        mesh=mesh,
        in_specs=placed,
        out_specs=(P("dp", "sp", None), P("dp", None), P("dp", None), P(), P(), P(), P()),
        check_vma=False,
    )
```

```python
import functools

import jax
import jax.numpy as jnp
from jax import lax
from jax.experimental import pallas as pl
from jax.experimental.pallas import tpu as pltpu
from jax.sharding import PartitionSpec as P

EPSILON = 1e-06
CORES = 2
MESH = pl.DeviceIdType.MESH
F32 = jnp.float32
BF16 = jnp.bfloat16


def remote(src, dst, send, recv, device):
    return pltpu.make_async_remote_copy(
        src_ref=src, dst_ref=dst, send_sem=send, recv_sem=recv, device_id=device, device_id_type=MESH
    )


def position():
    s, d = lax.axis_index("sp"), lax.axis_index("dp")
    return s, d, d // CORES, d % CORES


def greet(ways, levels, s, d, z, c):
    barrier = pltpu.get_barrier_semaphore()
    for k in range(1, ways):
        pl.semaphore_signal(barrier, inc=1, device_id=((s + k) % ways, d), device_id_type=MESH)
    for k in range(1, levels):
        other = ((z + k) % levels) * CORES + c
        pl.semaphore_signal(barrier, inc=1, device_id=(s, other), device_id_type=MESH)
    pl.semaphore_signal(barrier, inc=1, device_id=(s, d + 1 - 2 * c), device_id_type=MESH)
    pl.semaphore_wait(barrier, ways - 1 + levels - 1 + 1)


def phi(values):
    cdf_part = 0.5 * (1.0 + lax.erf(values * 0.7071067811865476))
    pdf_part = jnp.exp(-0.5 * values * values) * 0.3989422804014327
    return cdf_part, cdf_part + values * pdf_part


def kernel(
    ways, levels,
    tokens, weights, value_act, gate_act, cotangent, gain, shift, mix, mix_turned, bias,
    input_grad, summed, mix_out, small_out,
    both, peer_tokens, peer_grads, gathered, weight_grad, spatial_sum, gain_grad, shift_grad,
    own_part, swap_part, spread, low, spatial, grad_norm,
    part, mix_part, small,
    plane_in, level_out, level_in, own_sum, final, final_in,
    mix_in, mix_low, mix_plane, mix_sum, mix_level_out, mix_level, small_in, small_plane, small_level,
    pair_sem, shard_sem, spread_sem, relay_sem,
    core_sem, plane_sem, level_sem, gather_sem, mix_sem, mix_level_sem, mix_up_sem, mix_out_sem,
    small_sem, small_level_sem,
):
    s, d, z, c = position()
    partner = (s, d + 1 - 2 * c)
    seq_len, channels = value_act.shape
    pairs, double, block_len = mix.shape
    lanes = channels // pairs
    groups = 2 * pairs
    rows_own, width = weights.shape
    piece = width // ways
    model = tokens.shape[1]
    depth = model // levels

    def columns(index):
        return pl.ds(pl.multiple_of(index * piece, piece), piece)

    def in_plane(k):
        return ((s + k) % ways, d)

    def in_level(k):
        return (s, ((z + k) % levels) * CORES + c)

    greet(ways, levels, s, d, z, c)
    shard_copies = []
    for k in range(1, levels):
        shard_copies.append(remote(
            weights.at[:, columns(s)], gathered.at[z, c, :, columns(s)],
            shard_sem.at[0, k - 1], shard_sem.at[1, k - 1], in_level(k),
        ))
    order = sorted(range(levels - 1), key=lambda k: min(k + 1, levels - 1 - k))
    for k in order:
        shard_copies[k].start()
    token_swap = remote(tokens, peer_tokens, pair_sem.at[0, 0], pair_sem.at[1, 0], partner)
    token_swap.start()
    shard_swap = remote(weights, gathered.at[z, c], pair_sem.at[0, 1], pair_sem.at[1, 1], partner)
    shard_swap.start()

    spreads, relays = {}, {}

    def level_of(k):
        return (z + levels - 1 - k) % levels

    def forward(k):
        shard_copies[k].wait_recv()
        block = gathered.at[level_of(k), c, :, columns(s)]
        for j in range(1, ways):
            copy = remote(
                block, block, spread_sem.at[0, k, j - 1], spread_sem.at[1, k, j - 1], in_plane(j)
            )
            copy.start()
            spreads[k, j] = copy
        relay = remote(block, block, relay_sem.at[0, k, 0], relay_sem.at[1, k, 0], partner)
        relay.start()
        relays[k, 0] = relay

    def relay_all(k):
        for j in range(1, ways):
            spreads[k, j].wait_recv()
            block = gathered.at[level_of(k), c, :, columns((s + ways - j) % ways)]
            relay = remote(block, block, relay_sem.at[0, k, j], relay_sem.at[1, k, j], partner)
            relay.start()
            relays[k, j] = relay

    def project(shard, index):
        cut = pl.ds(pl.multiple_of(index * rows_own, rows_own), rows_own)
        input_grad[:, cut] = lax.dot_general(
            both[...], shard, (((1,), (1,)), ((), ())), preferred_element_type=F32
        ).astype(BF16)

    def project_level(k):
        level = level_of(k)
        for j in range(ways):
            relays[k, j].wait_recv()
        for core in range(CORES):
            project(gathered[level, core], level * CORES + core)

    weight_grad[...] = jnp.zeros_like(weight_grad)
    spatial_sum[...] = jnp.zeros_like(spatial_sum)
    gain_grad[...] = jnp.zeros_like(gain_grad)
    shift_grad[...] = jnp.zeros_like(shift_grad)
    lane = lax.broadcasted_iota(jnp.int32, (block_len, lanes), 1)
    first_half = lane < lanes // 2
    blocks = seq_len // block_len
    early, late = order[:blocks - 1], order[blocks - 1:]
    for b in range(blocks):
        rows = pl.ds(b * block_len, block_len)
        gate = gate_act[rows, :].astype(F32)
        gate_cdf, gate_slope = phi(gate)
        gelu = gate * gate_cdf
        centred = gelu - jnp.mean(gelu, axis=-1, keepdims=True)
        inv_std = lax.rsqrt(jnp.mean(centred * centred, axis=-1, keepdims=True) + EPSILON)
        normed = centred * inv_std
        spread[...] = (normed * gain[...] + shift[...]).astype(BF16)
        value = value_act[rows, :].astype(F32)
        value_cdf, value_slope = phi(value)
        grad_out = cotangent[rows, :].astype(F32)
        grad_spatial = grad_out * (value * value_cdf)
        spatial_sum[...] += grad_spatial
        low[...] = grad_spatial.astype(BF16)
        for p in range(pairs):
            cut = pl.ds(p * lanes, lanes)
            inner = spread[:, cut]
            mixed = jnp.dot(mix[p], inner, preferred_element_type=F32)
            spatial[:, cut] = jnp.where(first_half, mixed[:block_len], mixed[block_len:]) + bias[:, cut]
            piece_low = low[:, cut]
            zero = jnp.zeros_like(piece_low)
            apart = jnp.concatenate(
                (jnp.where(first_half, piece_low, zero), jnp.where(first_half, zero, piece_low)), axis=0
            )
            weight_grad[p] += lax.dot_general(
                apart, inner, (((1,), (1,)), ((), ())), preferred_element_type=F32
            )
            grad_norm[:, cut] = jnp.dot(mix_turned[p], apart, preferred_element_type=F32)
        back = grad_norm[...]
        gain_grad[...] += jnp.sum(back * normed, axis=0, keepdims=True)
        shift_grad[...] += jnp.sum(back, axis=0, keepdims=True)
        hat = back * gain[...]
        grad_gate = inv_std * (
            hat
            - jnp.mean(hat, axis=-1, keepdims=True)
            - normed * jnp.mean(hat * normed, axis=-1, keepdims=True)
        )
        value_grad = (grad_out * spatial[...] * value_slope).astype(BF16)
        gate_grad = (grad_gate * gate_slope).astype(BF16)
        both[rows, :channels] = value_grad
        both[rows, channels:] = gate_grad
        chosen = jnp.full(value_grad.shape, c, jnp.int32) == 0
        own_part[rows, :] = jnp.where(chosen, value_grad.astype(F32), gate_grad.astype(F32)).astype(BF16)
        swap_part[rows, :] = jnp.where(chosen, gate_grad.astype(F32), value_grad.astype(F32)).astype(BF16)
        if b < len(early):
            forward(early[b])
    grad_swap = remote(swap_part, peer_grads, pair_sem.at[0, 2], pair_sem.at[1, 2], partner)
    grad_swap.start()

    mix_part[...] = weight_grad[...].reshape(mix_part.shape)
    mix_swap = remote(mix_part.at[1 - c], mix_in, core_sem.at[0, 0], core_sem.at[1, 0], partner)
    mix_swap.start()
    sums = jnp.zeros((block_len, lanes), F32)
    for p in range(pairs):
        terms = spatial_sum[:, pl.ds(p * lanes, lanes)]
        lower = jnp.sum(jnp.where(first_half, terms, 0.0), axis=1, keepdims=True)
        upper = jnp.sum(jnp.where(first_half, 0.0, terms), axis=1, keepdims=True)
        sums = jnp.where(lane == 2 * p, lower, jnp.where(lane == 2 * p + 1, upper, sums))
    small[:groups, :] = sums.T[:groups]
    for p in range(pairs):
        cut = pl.ds(p * lanes, lanes)
        small[groups + p:groups + p + 1, :] = gain_grad[:, cut]
        small[groups + pairs + p:groups + pairs + p + 1, :] = shift_grad[:, cut]
    small_swap = remote(small, small_in, core_sem.at[0, 1], core_sem.at[1, 1], partner)
    small_swap.start()
    copies = {}
    token_swap.wait()
    grad_swap.wait()

    def send_chunk(i):
        target = (z + 1 + i) % levels
        cut = pl.ds(pl.multiple_of(target * depth, depth), depth)
        product = lax.dot_general(
            tokens[:, cut], own_part[...], (((0,), (0,)), ((), ())), preferred_element_type=F32
        ) + lax.dot_general(
            peer_tokens[:, cut], peer_grads[...], (((0,), (0,)), ((), ())), preferred_element_type=F32
        )
        part[i] = product.reshape(part.shape[1:]).astype(BF16)
        for k in range(1, ways):
            copy = remote(
                part.at[i, :, (s + k) % ways], plane_in.at[i, k - 1],
                plane_sem.at[0, i, k - 1], plane_sem.at[1, i, k - 1], in_plane(k),
            )
            copy.start()
            copies[i, k] = copy

    send_chunk(0)
    mix_swap.wait()
    small_swap.wait()
    mix_low[...] = (mix_part[c] + mix_in[...]).astype(BF16)
    small_plane[s] = small[...] + small_in[...]
    mix_copies, small_copies = [], []
    for k in range(1, ways):
        mix_copies.append(remote(
            mix_low.at[(s + k) % ways], mix_plane.at[k - 1],
            mix_sem.at[0, k - 1], mix_sem.at[1, k - 1], in_plane(k),
        ))
        small_copies.append(remote(
            small_plane.at[s], small_plane.at[s],
            small_sem.at[0, k - 1], small_sem.at[1, k - 1], in_plane(k),
        ))
    for copy in mix_copies + small_copies:
        copy.start()
    for i in range(1, levels):
        send_chunk(i)
    for k in late:
        forward(k)
    for k in early:
        relay_all(k)
    project(weights[...], d)
    shard_swap.wait()
    project(gathered[z, 1 - c], z * CORES + 1 - c)

    mix_level_copies, small_level_copies, mix_up, mix_gather = [], [], [], []

    def mix_stage(stage):
        if stage == 0:
            for copy in mix_copies + small_copies:
                copy.wait()
            total = mix_low[s].astype(F32)
            for k in range(1, ways):
                total = total + mix_plane[k - 1].astype(F32)
            mix_sum[...] = total
            mix_level_out[...] = total.astype(BF16)
            gathered_small = small_plane[0]
            for k in range(1, ways):
                gathered_small = gathered_small + small_plane[k]
            small_level[z] = gathered_small
            for k in range(1, levels):
                mix_level_copies.append(remote(
                    mix_level_out.at[(z + k) % levels], mix_level.at[k - 1],
                    mix_level_sem.at[0, k - 1], mix_level_sem.at[1, k - 1], in_level(k),
                ))
                small_level_copies.append(remote(
                    small_level.at[z], small_level.at[z],
                    small_level_sem.at[0, k - 1], small_level_sem.at[1, k - 1], in_level(k),
                ))
            for copy in mix_level_copies + small_level_copies:
                copy.start()
        elif stage == 1:
            for copy in mix_level_copies + small_level_copies:
                copy.wait()
            total = mix_sum[z]
            for k in range(1, levels):
                total = total + mix_level[k - 1].astype(F32)
            mix_out[c, s, z] = total.astype(BF16)
            gathered_small = small_level[0]
            for k in range(1, levels):
                gathered_small = gathered_small + small_level[k]
            small_out[...] = gathered_small
            for k in range(1, levels):
                block = mix_out.at[c, s, z]
                mix_up.append(remote(
                    block, block, mix_up_sem.at[0, k - 1], mix_up_sem.at[1, k - 1], in_level(k)
                ))
                mix_up[-1].start()
        else:
            for copy in mix_up:
                copy.wait()
            for k in range(1, ways):
                block = mix_out.at[c, s]
                mix_gather.append(remote(
                    block, block, mix_out_sem.at[0, k - 1], mix_out_sem.at[1, k - 1], in_plane(k)
                ))
                mix_gather[-1].start()

    stages = [0, 1, 2]
    level_copies = []
    for i in range(levels):
        total = part[i, :, s].astype(F32)
        for k in range(1, ways):
            copies[i, k].wait_recv()
            total = total + plane_in[i, k - 1].astype(F32)
        if i < levels - 1:
            level_out[i] = total.astype(BF16)
            copy = remote(
                level_out.at[i], level_in.at[i], level_sem.at[0, i], level_sem.at[1, i], in_level(i + 1)
            )
            copy.start()
            level_copies.append(copy)
            if stages:
                mix_stage(stages.pop(0))
            if i < len(early):
                project_level(early[i])
        else:
            own_sum[...] = total
    total = own_sum[...]
    for i in range(levels - 1):
        level_copies[i].wait_recv()
        total = total + level_in[i].astype(F32)
    final[...] = total
    final_swap = remote(final.at[1 - c], final_in, core_sem.at[0, 2], core_sem.at[1, 2], partner)
    final_swap.start()
    while stages:
        mix_stage(stages.pop(0))
    final_swap.wait()
    mine, theirs = final[c], final_in[...]
    lower_half = jnp.full(mine.shape, c, jnp.int32) == 0
    summed[s, :, :channels] = jnp.where(lower_half, mine, theirs).astype(BF16)
    summed[s, :, channels:] = jnp.where(lower_half, theirs, mine).astype(BF16)
    gather = []
    for k in range(1, ways):
        copy = remote(
            summed.at[s], summed.at[s], gather_sem.at[0, k - 1], gather_sem.at[1, k - 1], in_plane(k)
        )
        copy.start()
        gather.append(copy)
    for k in late:
        relay_all(k)
    for k in late:
        project_level(k)
    for copy in mix_gather:
        copy.wait()
    mix_back = remote(mix_out.at[c], mix_out.at[c], core_sem.at[0, 3], core_sem.at[1, 3], partner)
    mix_back.start()
    mix_back.wait()
    for copy in gather:
        copy.wait()
    for copy in level_copies + shard_copies:
        copy.wait_send()
    for pile in (copies, spreads, relays):
        for key in pile:
            pile[key].wait_send()


def shards(
    tokens,
    value_act,
    gate_act,
    cotangent,
    value_weight,
    gate_weight,
    norm_gain,
    norm_bias,
    mix_weight,
    mix_bias,
):
    ways = lax.axis_size("sp")
    levels = lax.axis_size("dp") // CORES
    inputs = tokens[0]
    seq_len, width = inputs.shape
    channels = value_act.shape[2]
    groups, block_len = mix_weight.shape[0], mix_weight.shape[1]
    group_dim = channels // groups
    pairs = groups // 2
    lanes = channels // pairs
    rows = value_weight.shape[0]
    share = rows // ways
    vmem = pl.BlockSpec(memory_space=pltpu.VMEM)
    sems = pltpu.SemaphoreType.DMA
    weights = jnp.concatenate((value_weight, gate_weight), axis=1)
    causal = jnp.tril(jnp.ones((block_len, block_len), dtype=bool))
    masked = jnp.where(causal[None], mix_weight, jnp.zeros_like(mix_weight))
    mix = masked.reshape(pairs, 2 * block_len, block_len)
    bias = jnp.repeat(mix_bias.T, group_dim, axis=1)
    low_rows = groups * block_len // (CORES * ways * levels)
    mix_shape = (CORES, ways, levels, low_rows, block_len)
    small_shape = (groups + 2 * pairs, lanes)
    shape = jax.ShapeDtypeStruct
    input_grad, summed, mix_out, small_out = pl.pallas_call(
        functools.partial(kernel, ways, levels),
        out_shape=(
            shape((seq_len, width), BF16),
            shape((ways, share, 2 * channels), BF16),
            shape(mix_shape, BF16),
            shape(small_shape, F32),
        ),
        in_specs=[vmem] * 10,
        out_specs=(vmem,) * 4,
        scratch_shapes=[
            pltpu.VMEM((seq_len, 2 * channels), BF16),
            pltpu.VMEM((seq_len, width), BF16),
            pltpu.VMEM((seq_len, channels), BF16),
            pltpu.VMEM((levels, CORES, rows, 2 * channels), BF16),
            pltpu.VMEM((pairs, 2 * block_len, block_len), F32),
            pltpu.VMEM((block_len, channels), F32),
            pltpu.VMEM((1, channels), F32),
            pltpu.VMEM((1, channels), F32),
            pltpu.VMEM((seq_len, channels), BF16),
            pltpu.VMEM((seq_len, channels), BF16),
            pltpu.VMEM((block_len, channels), BF16),
            pltpu.VMEM((block_len, channels), BF16),
            pltpu.VMEM((block_len, channels), F32),
            pltpu.VMEM((block_len, channels), F32),
            pltpu.VMEM((levels, CORES, ways, share, channels), BF16),
            pltpu.VMEM(mix_shape, F32),
            pltpu.VMEM(small_shape, F32),
            pltpu.VMEM((levels, ways - 1, CORES, share, channels), BF16),
            pltpu.VMEM((levels - 1, CORES, share, channels), BF16),
            pltpu.VMEM((levels - 1, CORES, share, channels), BF16),
            pltpu.VMEM((CORES, share, channels), F32),
            pltpu.VMEM((CORES, share, channels), F32),
            pltpu.VMEM((share, channels), F32),
            pltpu.VMEM(mix_shape[1:], F32),
            pltpu.VMEM(mix_shape[1:], BF16),
            pltpu.VMEM((ways - 1,) + mix_shape[2:], BF16),
            pltpu.VMEM(mix_shape[2:], F32),
            pltpu.VMEM(mix_shape[2:], BF16),
            pltpu.VMEM((levels - 1,) + mix_shape[3:], BF16),
            pltpu.VMEM(small_shape, F32),
            pltpu.VMEM((ways,) + small_shape, F32),
            pltpu.VMEM((levels,) + small_shape, F32),
            sems((2, 3)),
            sems((2, levels - 1)),
            sems((2, levels - 1, ways - 1)),
            sems((2, levels - 1, ways)),
            sems((2, 4)),
            sems((2, levels, ways - 1)),
            sems((2, levels - 1)),
            sems((2, ways - 1)),
            sems((2, ways - 1)),
            sems((2, levels - 1)),
            sems((2, levels - 1)),
            sems((2, ways - 1)),
            sems((2, ways - 1)),
            sems((2, levels - 1)),
        ],
        compiler_params=pltpu.CompilerParams(
            collective_id=0, has_side_effects=True, vmem_limit_bytes=60 * 1024 * 1024
        ),
        name="unit",
    )(
        inputs, weights, value_act[0], gate_act[0], cotangent[0],
        norm_gain[None], norm_bias[None], mix, mix.transpose(0, 2, 1), bias,
    )
    weight_sums = summed.reshape(rows, 2 * channels).astype(F32)
    mix_grad = jnp.where(causal[None], mix_out.reshape(groups, block_len, block_len).astype(F32), 0.0)
    small_out = small_out.reshape(-1)
    biases = groups * block_len
    return (
        input_grad[None],
        weight_sums[:, :channels],
        weight_sums[:, channels:],
        mix_grad,
        small_out[:biases].reshape(groups, block_len),
        small_out[biases:biases + channels],
        small_out[biases + channels:],
    )


def solution(mesh):
    placed = (
        P("dp", "sp", None),
        P("dp", "sp", None),
        P("dp", "sp", None),
        P("dp", "sp", None),
        P("dp", None),
        P("dp", None),
        P(),
        P(),
        P(),
        P(),
    )
    return jax.shard_map(
        shards,
        mesh=mesh,
        in_specs=placed,
        out_specs=(P("dp", "sp", None), P("dp", None), P("dp", None), P(), P(), P(), P()),
        check_vma=False,
    )
```
